256 devices in a mesh: ep: 64 (over z, x, core), tp: 4 (over y).
Axes of the slice: x: 4, y: 4, z: 8, core: 2. Of those that a mesh axis runs over, the one named last changes fastest.
Arguments:
- query_rows: bfloat16 [16384, 1024], P('ep', 'tp'), may hold values from -8 to 8
- key_rows: bfloat16 [16384, 256], P('ep', 'tp'), may hold values from -8 to 8
- value_rows: bfloat16 [16384, 256], P('ep', 'tp'), may hold values from -16 to 16
- query_gain: float32 [64], replicated, may hold values from 0.5 to 7.5
- key_gain: float32 [64], replicated, may hold values from 0.5 to 7.5
- moe_tokens: bfloat16 [32768, 2048], P(('ep', 'tp')), may hold values from -6 to 6
- norm_gain: float32 [2048], replicated, may hold values from 0.1 to 1.9
- routes: int32 [32768, 2], P('ep'), may hold values from 0 to 63, all different within a row; in each aligned block of 128 rows (0 to 127, 128 to 255, ...) at most 8 rows name the same one
- route_weights: float32 [32768, 2], P('ep'), may hold values from 0.1 to 1
- expert_gate: bfloat16 [64, 2048, 1024], P('ep', None, 'tp'), may hold values from -0.125 to 0.125
- expert_up: bfloat16 [64, 2048, 1024], P('ep', None, 'tp'), may hold values from -0.125 to 0.125
- expert_down: bfloat16 [64, 1024, 2048], P('ep', 'tp'), may hold values from -0.1875 to 0.1875
- shared_gate: bfloat16 [2048, 1024], P(None, 'tp'), may hold values from -0.125 to 0.125
- shared_up: bfloat16 [2048, 1024], P(None, 'tp'), may hold values from -0.125 to 0.125
- shared_down: bfloat16 [1024, 2048], P('tp'), may hold values from -0.1875 to 0.1875
Outputs:
- attn_out: bfloat16 [16384, 1024], P('ep', 'tp')
- moe_out: bfloat16 [32768, 2048], P(('ep', 'tp'))
The draws below stay inside these ranges and needn't reach their ends.
Inputs may be any that keep to these rules, and one draw needn't show every extreme that they name: `routes`: each row names 2 different experts. Within each aligned block of 128 rows no expert is named more than 8 times, and in every draw some expert is named exactly 8 times in some block.
All inputs are finite; a program needn't handle non-finite values.
Results may differ from the reference program's by a relative error of at most 0.012.
The reference program's roundings to bfloat16 on the way count: a program that leaves them out, or rounds other values in their place, can miss the bound.
Values may be sent and summed in bfloat16 or wider, within the bound.
No kernel may reach another device: no remote copies, remote signals or barrier semaphores. Data moves between devices by JAX's collectives and lax.ppermute only.
A program may use at most 192 MiB of HBM per device.

```python
import math
import jax
import jax.numpy as jnp
import numpy as np
from jax import lax

D = 2048
HEADS = 16
KV_HEADS = 4
HD = 64
F = 1024
TOP = 2
GRID_W = 64
TOK_B = 128
TOKENS_A = 16384
TOKENS_B = 32768
EXPERTS = 64
CAP = 8
N_TP = 4


def draw_key_rows(key, part):
    result = jnp.clip(jax.random.normal(jax.random.fold_in(key, 72), (TOKENS_A, KV_HEADS * HD), jnp.float32), -6.0, 6.0)
    return result.astype(jnp.bfloat16)


def draw_query_rows(key, part):
    result = jnp.clip(jax.random.normal(jax.random.fold_in(key, 73), (TOKENS_A, HEADS * HD), jnp.float32), -6.0, 6.0)
    return result.astype(jnp.bfloat16)


def gain_draw(key, salt):
    result = jax.random.uniform(jax.random.fold_in(key, salt + 3), (HD,), jnp.float32, 1.2, 1.8)
    return result


def draw_query_gain(key, part):
    return gain_draw(key, 80)


def draw_key_gain(key, part):
    return gain_draw(key, 90)


def level_of(key, dims, pieces, low, top_value):
    factor_of, own = 1.0, jax.random.fold_in(key, 6)
    for axis_at, blocks in pieces:
        heights = jnp.exp(jax.random.uniform(jax.random.fold_in(own, axis_at), (blocks,), jnp.float32, low / len(pieces), top_value / len(pieces)))
        factor_of = factor_of * jnp.repeat(heights, dims[axis_at] // blocks).reshape([-1 if axis == axis_at else 1 for axis in range(len(dims))])
    return factor_of


def assign_block(stream_key, own, number, rows, amount, top, bound, slope):
    ranking = jax.random.permutation(stream_key, amount)
    crowded, common = portions_of(amount, rows * top, bound, slope, True), portions_of(amount, rows * top, bound, slope, False)
    places = jnp.arange(amount)

    def named(sizes, rotation):
        used = int((sizes > 0).sum())
        fixed = max(1, used // 4)
        passed = fixed + (places - fixed + rotation * (used - fixed)) % max(1, amount - fixed)
        return jnp.zeros((amount,), jnp.int32).at[ranking[jnp.where(places < fixed, places, passed)]].set(jnp.asarray(sizes, jnp.int32))

    sizes = jnp.where(number % 4 == 0, named(crowded, number // 4), named(common, number - number // 4 - 1))
    mixed = jax.random.permutation(jax.random.fold_in(own, 3), amount)
    source_of, receiver = mixed[0:amount // 2 * 2:2], mixed[1:amount // 2 * 2:2]
    room = jnp.minimum(sizes[source_of] - 1, bound - sizes[receiver]) // 2
    room = jnp.where((source_of == ranking[0]) | (receiver == ranking[0]) | (sizes[receiver] == 0), 0, jnp.maximum(room, 0))
    passed = jax.random.randint(jax.random.fold_in(own, 4), (amount // 2,), 0, 1 << 20) % (room + 1)
    sizes = sizes.at[source_of].add(-passed).at[receiver].add(passed)
    items = jnp.searchsorted(jnp.cumsum(sizes), jnp.arange(rows * top), side="right").astype(jnp.int32)
    table = items.reshape(top, rows).T
    table = table[jax.random.permutation(jax.random.fold_in(own, 1), rows)]
    rotation = jax.random.randint(jax.random.fold_in(own, 2), (rows, 1), 0, top)
    return jnp.take_along_axis(table, (jnp.arange(top)[None, :] + rotation) % top, axis=1)


def portions_of(number_of, total, limit, skew, full):
    weights = [(1 << 20) // math.isqrt(standing ** skew) + 1 for standing in range(1, number_of + 1)]
    largest = limit if full else min(limit, max(-(-total // number_of), total * weights[0] // sum(weights)))
    least = 1 if total - largest >= number_of - 1 else 0
    holding, surplus = [largest] + [least] * (number_of - 1), total - largest - least * (number_of - 1)
    while surplus > 0:
        movable = [i for i in range(1, number_of) if holding[i] < largest] or [i for i in range(1, number_of) if holding[i] < limit]
        pool, remaining = sum([weights[i] for i in movable]), surplus
        for i in movable:
            more = min(limit - holding[i], max(1, remaining * weights[i] // pool), surplus)
            holding[i] = holding[i] + more
            surplus = surplus - more
    return np.array(holding)


def gaussian(key, extent, width, reach, pieces=(), kind=jnp.bfloat16):
    entries = width * jax.random.normal(key, extent, jnp.float32)
    if pieces:
        entries = entries * level_of(key, extent, pieces, -0.22, 0.18)
    return jnp.clip(entries, -reach, reach).astype(kind)


def setup_inputs(seed: int = 0) -> dict:
    key_list = jax.random.split(jax.random.key(seed), 16)
    query_rows = draw_query_rows(jax.random.fold_in(key_list[15], 71), 0)
    key_rows = draw_key_rows(jax.random.fold_in(key_list[15], 71), 0)
    value_rows = gaussian(key_list[2], (TOKENS_A, KV_HEADS * HD), 3.0, 16.0, ((0, 64), (1, 4)))
    query_gain = draw_query_gain(jax.random.fold_in(key_list[15], 71), 0)
    key_gain = draw_key_gain(jax.random.fold_in(key_list[15], 71), 0)
    moe_tokens = gaussian(key_list[5], (TOKENS_B, D), 1.0, 6.0, ((0, 256),))
    norm_gain = jnp.clip(1.0 + 0.18 * jax.random.normal(key_list[6], (D,), jnp.float32), 0.1, 1.9)
    routes_keys = jax.random.split(jax.random.fold_in(key_list[7], 1), TOKENS_B // TOK_B)
    routes_turns = jax.random.permutation(jax.random.fold_in(key_list[7], 3), TOKENS_B // TOK_B)
    routes = jax.vmap(lambda own, number: assign_block(jax.random.fold_in(key_list[7], 2), own, number, TOK_B, EXPERTS, TOP, CAP, 1))(routes_keys, routes_turns).reshape((TOKENS_B, TOP))
    route_weights = jnp.clip(0.1 + 0.9 * jax.random.uniform(key_list[8], (TOKENS_B, TOP), jnp.float32) ** level_of(key_list[8], (TOKENS_B, TOP), ((0, 64),), -0.2, 0.2), 0.1, 1.0)
    expert_gate = gaussian(key_list[9], (EXPERTS, D, F), D ** -0.5, 0.125, ((0, 64), (2, 4)))
    expert_up = gaussian(key_list[10], (EXPERTS, D, F), D ** -0.5, 0.125, ((0, 64), (2, 4)))
    expert_down = gaussian(key_list[11], (EXPERTS, F, D), F ** -0.5, 0.1875, ((0, 64), (1, 4)))
    shared_gate = gaussian(key_list[12], (D, F), D ** -0.5, 0.125, ((1, 4),))
    shared_up = gaussian(key_list[13], (D, F), D ** -0.5, 0.125, ((1, 4),))
    shared_down = gaussian(key_list[14], (F, D), F ** -0.5, 0.1875, ((0, 4),))
    return {"query_rows": query_rows, "key_rows": key_rows, "value_rows": value_rows, "query_gain": query_gain, "key_gain": key_gain, "moe_tokens": moe_tokens, "norm_gain": norm_gain, "routes": routes, "route_weights": route_weights, "expert_gate": expert_gate, "expert_up": expert_up, "expert_down": expert_down, "shared_gate": shared_gate, "shared_up": shared_up, "shared_down": shared_down}


epsilon = 1e-06
rotary_base = 10000.0
routed_scale = 2.5

def rotate_heads(heads_in, gain_row, positions):
    values32 = heads_in.astype(jnp.float32)
    scaled = values32 * lax.rsqrt(lax.optimization_barrier(jnp.mean(values32 * values32, axis=-1, keepdims=True)) + epsilon) * gain_row
    pair_count = scaled.shape[-1] // 4
    inv_freq = rotary_base ** (-jnp.arange(pair_count, dtype=jnp.float32) / pair_count)
    grid_row = (positions // GRID_W).astype(jnp.float32)
    grid_col = (positions % GRID_W).astype(jnp.float32)
    angles = jnp.concatenate([grid_row[:, None] * inv_freq, grid_col[:, None] * inv_freq], axis=-1)[:, None, :]
    cosine = jnp.cos(angles)
    sine_part = jnp.sin(angles)
    first_half = scaled[..., 0::2]
    second_half = scaled[..., 1::2]
    turned = jnp.stack([first_half * cosine - second_half * sine_part, first_half * sine_part + second_half * cosine], axis=-1)
    return turned.reshape(scaled.shape).astype(jnp.bfloat16)

def attention(query_rows, key_rows, value_rows, query_gain, key_gain):
    token_count = query_rows.shape[0]
    group = HEADS // KV_HEADS
    positions = jnp.arange(token_count, dtype=jnp.int32)
    q_rot = rotate_heads(query_rows.reshape(token_count, HEADS, HD), query_gain, positions)
    k_rot = rotate_heads(key_rows.reshape(token_count, KV_HEADS, HD), key_gain, positions)
    keys32 = lax.optimization_barrier(k_rot).astype(jnp.float32)
    values32 = value_rows.reshape(token_count, KV_HEADS, HD).astype(jnp.float32)
    block_len = math.gcd(token_count, 256)
    q_blocks = lax.optimization_barrier(q_rot).reshape(token_count // block_len, block_len, KV_HEADS, group, HD)

    def one_block(q_block):
        scores = jnp.einsum('qgrd,sgd->qgrs', q_block.astype(jnp.float32), keys32) * HD ** (-0.5)
        row_max = lax.optimization_barrier(jnp.max(scores, axis=-1, keepdims=True))
        weights = jnp.exp(scores - row_max)
        row_sum = lax.optimization_barrier(jnp.sum(weights, axis=-1, keepdims=True))
        rounded = lax.optimization_barrier(weights.astype(jnp.bfloat16)).astype(jnp.float32)
        mixed = jnp.einsum('qgrs,sgd->qgrd', rounded, values32)
        return (mixed / row_sum).astype(jnp.bfloat16)
    result = lax.map(one_block, q_blocks)
    return result.reshape(token_count, HEADS * HD)

def feed_forward(rows_in, w_gate, w_up, w_down):
    gate_proj = jnp.dot(rows_in, w_gate, preferred_element_type=jnp.float32)
    up_proj = jnp.dot(rows_in, w_up, preferred_element_type=jnp.float32)
    hidden = lax.optimization_barrier((jax.nn.silu(gate_proj) * up_proj).astype(jnp.bfloat16))
    block_width = hidden.shape[-1] // N_TP
    summed = jnp.zeros((rows_in.shape[0], w_down.shape[1]), jnp.float32)
    for part_index in range(N_TP):
        lower = part_index * block_width
        partial_sum = jnp.dot(hidden[:, lower:lower + block_width], w_down[lower:lower + block_width], preferred_element_type=jnp.float32).astype(jnp.bfloat16)
        summed = summed + lax.optimization_barrier(partial_sum).astype(jnp.float32)
    return summed

def mixture(moe_tokens, norm_gain, routes, route_weights, expert_gate, expert_up, expert_down, shared_gate, shared_up, shared_down):
    total_rows = moe_tokens.shape[0]
    blocks = total_rows // TOK_B
    values32 = moe_tokens.astype(jnp.float32)
    normed = (values32 * lax.rsqrt(lax.optimization_barrier(jnp.mean(values32 * values32, axis=-1, keepdims=True)) + epsilon) * norm_gain).astype(jnp.bfloat16)
    normed = lax.optimization_barrier(normed)
    gates = route_weights / lax.optimization_barrier(jnp.sum(route_weights, axis=-1, keepdims=True)) * routed_scale
    chosen = routes.reshape(blocks, TOK_B * TOP).astype(jnp.int32)
    one_hot = (chosen[:, :, None] == jnp.arange(EXPERTS, dtype=jnp.int32)[None, None, :]).astype(jnp.int32)
    ranks = lax.optimization_barrier(jnp.sum((jnp.cumsum(one_hot, axis=1) - one_hot) * one_hot, axis=2))
    block_ids = jnp.arange(blocks, dtype=jnp.int32)[:, None]
    dest = (chosen * blocks + block_ids) * CAP + ranks
    rows_from = block_ids * TOK_B + jnp.arange(TOK_B * TOP, dtype=jnp.int32)[None, :] // TOP
    slot_rows = jnp.full((EXPERTS * blocks * CAP,), total_rows, jnp.int32).at[dest.reshape(-1)].set(rows_from.reshape(-1))
    padded = jnp.concatenate([normed, jnp.zeros((1, D), jnp.bfloat16)], axis=0)

    def one_expert(inputs):
        index_rows, w_gate, w_up, w_down = inputs
        return feed_forward(padded[index_rows], w_gate, w_up, w_down).astype(jnp.bfloat16)
    expert_rows = lax.map(one_expert, (slot_rows.reshape(EXPERTS, blocks * CAP), expert_gate, expert_up, expert_down))
    flat_rows = lax.optimization_barrier(expert_rows.reshape(EXPERTS * blocks * CAP, D))
    picked = flat_rows[dest.reshape(-1)].astype(jnp.float32).reshape(total_rows, TOP, D)
    routed = lax.optimization_barrier(jnp.sum(gates[:, :, None] * picked, axis=1))
    shared = feed_forward(normed, shared_gate, shared_up, shared_down)
    return (routed + shared).astype(jnp.bfloat16)

def reference(query_rows, key_rows, value_rows, query_gain, key_gain, moe_tokens, norm_gain, routes, route_weights, expert_gate, expert_up, expert_down, shared_gate, shared_up, shared_down):
    attn_out = attention(query_rows, key_rows, value_rows, query_gain, key_gain)
    moe_out = mixture(moe_tokens, norm_gain, routes, route_weights, expert_gate, expert_up, expert_down, shared_gate, shared_up, shared_down)
    return (attn_out, moe_out)
```

```python
import functools

import jax
import jax.numpy as jnp
from jax import lax
from jax.experimental import pallas as pl
from jax.experimental.pallas import tpu as pltpu
from jax.sharding import Mesh
from jax.sharding import PartitionSpec as P

GRID_W = 64
EP = ("ep_0", "ep_1", "ep_2")
EP_TP = ("ep_0", "ep_1", "ep_2", "tp")


epsilon = 1e-06
rotary_base = 10000.0
routed_scale = 2.5


def copy_for_each(array, axis):
    count = lax.axis_size(axis)
    return lax.all_to_all(
        jnp.broadcast_to(array[None], (count, *array.shape)), axis, 0, 0, tiled=True
    )


def rotate_heads(heads_in, gain_row, positions):
    values32 = heads_in.astype(jnp.float32)
    scaled = (
        values32
        * lax.rsqrt(jnp.mean(values32 * values32, axis=-1, keepdims=True) + epsilon)
        * gain_row
    )
    pair_count = scaled.shape[-1] // 4
    inv_freq = rotary_base ** (-jnp.arange(pair_count, dtype=jnp.float32) / pair_count)
    grid_row = (positions // GRID_W).astype(jnp.float32)
    grid_col = (positions % GRID_W).astype(jnp.float32)
    angles = jnp.concatenate([grid_row[:, None] * inv_freq, grid_col[:, None] * inv_freq], axis=-1)[
        :, None, :
    ]
    cosine = jnp.cos(angles)
    sine_part = jnp.sin(angles)
    first_half = scaled[..., 0::2]
    second_half = scaled[..., 1::2]
    turned = jnp.stack(
        [
            first_half * cosine - second_half * sine_part,
            first_half * sine_part + second_half * cosine,
        ],
        axis=-1,
    )
    return turned.reshape(scaled.shape).astype(jnp.bfloat16)


def flash_kernel(q_ref, kv_ref, out_ref, max_ref, sum_ref, acc_ref, *, scale, rows):
    step = pl.program_id(0)

    @pl.when(step == 0)
    def _():
        max_ref[...] = jnp.full(max_ref.shape, -jnp.inf, jnp.float32)
        sum_ref[...] = jnp.zeros(sum_ref.shape, jnp.float32)
        acc_ref[...] = jnp.zeros(acc_ref.shape, jnp.float32)

    kv = kv_ref[...]
    for part in range(q_ref.shape[0] // rows):
        at = pl.ds(part * rows, rows)
        scores = (
            lax.dot_general(
                q_ref[at, :], kv, (((1,), (1,)), ((), ())), preferred_element_type=jnp.float32
            )
            * scale
        )
        old_max = max_ref[at, :]
        new_max = jnp.maximum(old_max, jnp.max(scores, axis=1, keepdims=True))
        factor = jnp.exp(old_max - new_max)
        weights = jnp.exp(scores - new_max)
        sum_ref[at, :] = sum_ref[at, :] * factor + jnp.sum(weights, axis=1, keepdims=True)
        acc_ref[at, :] = acc_ref[at, :] * factor + jnp.dot(
            weights.astype(jnp.bfloat16), kv, preferred_element_type=jnp.float32
        )
        max_ref[at, :] = new_max

    @pl.when(step == pl.num_programs(0) - 1)
    def _():
        out_ref[...] = (acc_ref[...] / sum_ref[...]).astype(jnp.bfloat16)


def flash(q_padded, key_value, head_size, span, rows):
    query_count, width = q_padded.shape
    key_count = key_value.shape[0]
    return pl.pallas_call(
        functools.partial(flash_kernel, scale=head_size ** (-0.5), rows=rows),
        grid=(key_count // span,),
        in_specs=[
            pl.BlockSpec((query_count, width), lambda i: (0, 0)),
            pl.BlockSpec((span, width), lambda i: (i, 0)),
        ],
        out_specs=pl.BlockSpec((query_count, width), lambda i: (0, 0)),
        out_shape=jax.ShapeDtypeStruct((query_count, width), jnp.bfloat16),
        scratch_shapes=[
            pltpu.VMEM((query_count, 1), jnp.float32),
            pltpu.VMEM((query_count, 1), jnp.float32),
            pltpu.VMEM((query_count, width), jnp.float32),
        ],
        compiler_params=pltpu.CompilerParams(dimension_semantics=("arbitrary",)),
        cost_estimate=pl.CostEstimate(
            flops=8 * query_count * key_count * width,
            bytes_accessed=2 * key_count * width,
            transcendentals=query_count * key_count,
        ),
        name="flash",
    )(q_padded, key_value)


def attend(query_rows, key_rows, value_rows, query_gain, key_gain):
    row_count = query_rows.shape[0]
    head_size = query_gain.shape[0]
    group = query_rows.shape[1] // head_size
    positions = lax.axis_index(EP) * row_count + jnp.arange(row_count, dtype=jnp.int32)
    k_rot = rotate_heads(key_rows.reshape(row_count, 1, head_size), key_gain, positions)
    key_value = jnp.concatenate([k_rot.reshape(row_count, head_size), value_rows], axis=1)
    for axis in ("ep_0", "ep_1", "ep_2"):
        with jax.named_scope("kv_" + axis):
            key_value = copy_for_each(key_value, axis)
    key_value = key_value.reshape(-1, 2 * head_size)
    q_rot = rotate_heads(query_rows.reshape(row_count, group, head_size), query_gain, positions)
    q_padded = jnp.concatenate([q_rot, jnp.zeros_like(q_rot)], axis=-1).transpose(1, 0, 2)
    q_padded = q_padded.reshape(group * row_count, 2 * head_size)
    result = flash(q_padded, key_value, head_size, 2048, 256)
    result = result[:, head_size:].reshape(group, row_count, head_size).transpose(1, 0, 2)
    return result.reshape(row_count, group * head_size)


def slots_of(routes, experts, capacity):
    tokens, top_count = routes.shape
    expert_ids = lax.broadcasted_iota(jnp.int32, (tokens, experts), 1)
    named = [(routes[:, k : k + 1] == expert_ids).astype(jnp.float32) for k in range(top_count)]
    earlier = (
        lax.broadcasted_iota(jnp.int32, (tokens, tokens), 1)
        < lax.broadcasted_iota(jnp.int32, (tokens, tokens), 0)
    ).astype(jnp.bfloat16)
    before = jnp.dot(
        earlier, sum(named).astype(jnp.bfloat16), preferred_element_type=jnp.float32
    )
    slot_ids = lax.broadcasted_iota(jnp.int32, (tokens, experts * capacity), 1)
    result = []
    for k in range(top_count):
        rank = jnp.sum(before * named[k], axis=1, keepdims=True).astype(jnp.int32)
        slot = routes[:, k : k + 1] * capacity + rank
        result.append((slot == slot_ids).astype(jnp.float32))
    return result


def dispatch_kernel(tokens_ref, gain_ref, routes_ref, send_ref, normed_ref, *, experts, capacity):
    values32 = tokens_ref[...].astype(jnp.float32)
    normed = (
        values32
        * lax.rsqrt(jnp.mean(values32 * values32, axis=-1, keepdims=True) + epsilon)
        * gain_ref[...]
    ).astype(jnp.bfloat16)
    normed_ref[...] = normed
    chosen = sum(slots_of(routes_ref[...], experts, capacity)).T.astype(jnp.bfloat16)
    send_ref[...] = jnp.dot(chosen, normed, preferred_element_type=jnp.float32).astype(
        jnp.bfloat16
    )


def combine_kernel(
    routes_ref, weights_ref, returned_ref, shared_ref, out_ref, *, experts, capacity
):
    weights = weights_ref[...]
    gates = weights / jnp.sum(weights, axis=-1, keepdims=True) * routed_scale
    returned = returned_ref[...]
    total = jnp.zeros(out_ref.shape, jnp.float32)
    for k, chosen in enumerate(slots_of(routes_ref[...], experts, capacity)):
        picked = jnp.dot(
            chosen.astype(jnp.bfloat16), returned, preferred_element_type=jnp.float32
        )
        total = total + gates[:, k : k + 1] * picked
    shared = shared_ref[0].astype(jnp.float32)
    for k in range(1, shared_ref.shape[0]):
        shared = shared + shared_ref[k].astype(jnp.float32)
    out_ref[...] = (total + shared).astype(jnp.bfloat16)


def shared_products(rows_in, w_gate, w_up, w_down):
    gate_proj = jnp.dot(rows_in, w_gate, preferred_element_type=jnp.float32)
    up_proj = jnp.dot(rows_in, w_up, preferred_element_type=jnp.float32)
    hidden = (jax.nn.silu(gate_proj) * up_proj).astype(jnp.bfloat16)
    return jnp.dot(hidden, w_down, preferred_element_type=jnp.float32)


def experts_half(
    moe_tokens,
    norm_gain,
    routes,
    route_weights,
    expert_gate,
    expert_up,
    expert_down,
    shared_gate,
    shared_up,
    shared_down,
):
    tok_rows, model_width = moe_tokens.shape
    top_count = routes.shape[1]
    experts = expert_gate.shape[0] * lax.axis_size(EP)
    capacity = 2 * tok_rows * top_count // experts
    slots = experts * capacity
    lane = lax.axis_index("tp")
    own_routes = lax.dynamic_slice_in_dim(routes, lane * tok_rows, tok_rows, 0)
    own_weights = lax.dynamic_slice_in_dim(route_weights, lane * tok_rows, tok_rows, 0)

    with jax.named_scope("weights"):
        gate_all = lax.all_gather(expert_gate[0], "tp")
        up_all = lax.all_gather(expert_up[0], "tp")
        down_all = lax.all_gather(expert_down[0], "tp")

    send, normed = pl.pallas_call(
        functools.partial(dispatch_kernel, experts=experts, capacity=capacity),
        out_shape=(
            jax.ShapeDtypeStruct((slots, model_width), jnp.bfloat16),
            jax.ShapeDtypeStruct((tok_rows, model_width), jnp.bfloat16),
        ),
        name="dispatch",
    )(moe_tokens, norm_gain[None], own_routes)

    with jax.named_scope("send_rows"):
        arrived = lax.all_to_all(
            send.reshape(experts, capacity, model_width), EP, 0, 0, tiled=True
        )
    arrived = arrived.reshape(slots, model_width)

    with jax.named_scope("shared_rows"):
        group_rows = copy_for_each(normed, "tp").reshape(-1, model_width)
    shared_part = shared_products(group_rows, shared_gate, shared_up, shared_down)
    with jax.named_scope("shared_back"):
        shared_parts = lax.all_to_all(
            shared_part.astype(jnp.bfloat16).reshape(-1, tok_rows, model_width),
            "tp",
            0,
            0,
            tiled=True,
        )

    gate_proj = jnp.einsum("rd,qdf->qrf", arrived, gate_all, preferred_element_type=jnp.float32)
    up_proj = jnp.einsum("rd,qdf->qrf", arrived, up_all, preferred_element_type=jnp.float32)
    hidden = (jax.nn.silu(gate_proj) * up_proj).astype(jnp.bfloat16)
    partial = jnp.einsum("qrf,qfd->qrd", hidden, down_all, preferred_element_type=jnp.float32)
    outgoing = jnp.sum(partial.astype(jnp.bfloat16).astype(jnp.float32), axis=0)
    with jax.named_scope("return_rows"):
        returned = lax.all_to_all(
            outgoing.astype(jnp.bfloat16).reshape(experts, capacity, model_width),
            EP,
            0,
            0,
            tiled=True,
        )
    return pl.pallas_call(
        functools.partial(combine_kernel, experts=experts, capacity=capacity),
        out_shape=jax.ShapeDtypeStruct((tok_rows, model_width), jnp.bfloat16),
        name="combine",
    )(own_routes, own_weights, returned.reshape(slots, model_width), shared_parts)


def body(
    query_rows,
    key_rows,
    value_rows,
    query_gain,
    key_gain,
    moe_tokens,
    norm_gain,
    routes,
    route_weights,
    expert_gate,
    expert_up,
    expert_down,
    shared_gate,
    shared_up,
    shared_down,
):
    attn_out = attend(query_rows, key_rows, value_rows, query_gain, key_gain)
    moe_out = experts_half(
        moe_tokens,
        norm_gain,
        routes,
        route_weights,
        expert_gate,
        expert_up,
        expert_down,
        shared_gate,
        shared_up,
        shared_down,
    )
    return (attn_out, moe_out)


def solution(mesh):
    finer = Mesh(mesh.devices.reshape(8, 4, 2, mesh.shape["tp"]), ("ep_0", "ep_1", "ep_2", "tp"))
    return jax.shard_map(
        body,
        mesh=finer,
        in_specs=(
            P(EP, "tp"),
            P(EP, "tp"),
            P(EP, "tp"),
            P(),
            P(),
            P(EP_TP, None),
            P(),
            P(EP, None),
            P(EP, None),
            P(EP, None, "tp"),
            P(EP, None, "tp"),
            P(EP, "tp", None),
            P(None, "tp"),
            P(None, "tp"),
            P("tp", None),
        ),
        out_specs=(P(EP, "tp"), P(EP_TP, None)),
        check_vma=False,
    )
```

```python
import functools
import math

import jax
import jax.numpy as jnp
from jax import lax
from jax.experimental import pallas as pl
from jax.sharding import Mesh
from jax.sharding import PartitionSpec as P


GRID_W = 64
EP = ("ep_0", "ep_1", "ep_2")
EP_TP = ("ep_0", "ep_1", "ep_2", "tp")


epsilon = 1e-06
rotary_base = 10000.0
routed_scale = 2.5

PARTS = 1


def shifted(array, axis, by):
    count = lax.axis_size(axis)
    return lax.ppermute(array, axis, [(i, (i + by) % count) for i in range(count)])


def rotate_heads(heads_in, gain_row, positions):
    values32 = heads_in.astype(jnp.float32)
    scaled = (
        values32
        * lax.rsqrt(jnp.mean(values32 * values32, axis=-1, keepdims=True) + epsilon)
        * gain_row
    )
    pair_count = scaled.shape[-1] // 4
    inv_freq = rotary_base ** (-jnp.arange(pair_count, dtype=jnp.float32) / pair_count)
    grid_row = (positions // GRID_W).astype(jnp.float32)
    grid_col = (positions % GRID_W).astype(jnp.float32)
    angles = jnp.concatenate([grid_row[:, None] * inv_freq, grid_col[:, None] * inv_freq], axis=-1)[
        :, None, :
    ]
    cosine = jnp.cos(angles)
    sine_part = jnp.sin(angles)
    first_half = scaled[..., 0::2]
    second_half = scaled[..., 1::2]
    turned = jnp.stack(
        [
            first_half * cosine - second_half * sine_part,
            first_half * sine_part + second_half * cosine,
        ],
        axis=-1,
    )
    return turned.reshape(scaled.shape).astype(jnp.bfloat16)


def flash_kernel(*refs, scale, rows, pieces, first, last):
    q_ref, kv_refs, refs = refs[0], refs[1 : 1 + pieces], refs[1 + pieces :]
    if not first:
        max_in, sum_in, acc_in = refs[:3]
        refs = refs[3:]
    factor_of = scale * math.log2(math.e)

    def scores_of(at, kv_ref):
        return lax.dot_general(
            q_ref[at, :], kv_ref[...], (((1,), (1,)), ((), ())), preferred_element_type=jnp.float32
        )

    def some_rows(step, unused):
        at = pl.ds(pl.multiple_of(step * rows, rows), rows)
        if first:
            run_max = jnp.full((rows, 1), -jnp.inf, jnp.float32)
            run_sum = jnp.zeros((rows, 1), jnp.float32)
            mixed = jnp.zeros((rows, q_ref.shape[1]), jnp.float32)
        else:
            run_max, run_sum, mixed = max_in[at, :], sum_in[at, :], acc_in[at, :]
        scores = scores_of(at, kv_refs[0])
        for k, kv_ref in enumerate(kv_refs):
            later = scores_of(at, kv_refs[k + 1]) if k + 1 < pieces else None
            new_max = jnp.maximum(run_max, jnp.max(scores, axis=1, keepdims=True))
            weights = jnp.exp2((scores - new_max) * factor_of)
            factor = jnp.exp2((run_max - new_max) * factor_of)
            run_sum = run_sum * factor + jnp.sum(weights, axis=1, keepdims=True)
            mixed = mixed * factor + jnp.dot(
                weights.astype(jnp.bfloat16), kv_ref[...], preferred_element_type=jnp.float32
            )
            run_max, scores = new_max, later
        if last:
            refs[0][at, :] = (mixed / run_sum).astype(jnp.bfloat16)
        else:
            refs[0][at, :], refs[1][at, :], refs[2][at, :] = run_max, run_sum, mixed
        return unused

    lax.fori_loop(0, q_ref.shape[0] // rows, some_rows, 0)


def flash(q_padded, pieces, state, last, scale):
    query_count, width = q_padded.shape
    column = jax.ShapeDtypeStruct((query_count, 1), jnp.float32)
    if last:
        out_shape = jax.ShapeDtypeStruct((query_count, width), jnp.bfloat16)
    else:
        out_shape = (column, column, jax.ShapeDtypeStruct((query_count, width), jnp.float32))
    keys = sum(piece.shape[0] for piece in pieces)
    return pl.pallas_call(
        functools.partial(
            flash_kernel,
            scale=scale,
            rows=256,
            pieces=len(pieces),
            first=state is None,
            last=last,
        ),
        out_shape=out_shape,
        cost_estimate=pl.CostEstimate(
            flops=8 * query_count * keys * width,
            bytes_accessed=2 * keys * width,
            transcendentals=query_count * keys,
        ),
        name="flash",
    )(q_padded, *pieces, *(state or ()))


def attend(query_rows, key_rows, value_rows, query_gain, key_gain):
    row_count = query_rows.shape[0]
    head_size = query_gain.shape[0]
    group = query_rows.shape[1] // head_size
    positions = lax.axis_index(EP) * row_count + jnp.arange(row_count, dtype=jnp.int32)
    k_rot = rotate_heads(key_rows.reshape(row_count, 1, head_size), key_gain, positions)
    own = jnp.concatenate([k_rot.reshape(row_count, head_size), value_rows], axis=1)
    copies = jnp.broadcast_to(own[None], (lax.axis_size("ep_0"), *own.shape))
    column = lax.all_to_all(copies, "ep_0", 0, 0, tiled=True)
    column = column.reshape(-1, own.shape[1])
    pieces = [column]
    for by in range(1, lax.axis_size("ep_1")):
        pieces.append(shifted(column, "ep_1", by))
    peers = [shifted(piece, "ep_2", 1) for piece in pieces]
    q_rot = rotate_heads(query_rows.reshape(row_count, group, head_size), query_gain, positions)
    q_padded = jnp.concatenate([q_rot, jnp.zeros_like(q_rot)], axis=-1).transpose(1, 0, 2)
    q_padded = q_padded.reshape(group * row_count, 2 * head_size)
    scale = head_size ** (-0.5)
    state = None
    for k, some in enumerate((pieces[:2], pieces[2:], peers[:2], peers[2:])):
        state = flash(q_padded, some, state, k == 3, scale)
    result = state[:, head_size:].reshape(group, row_count, head_size).transpose(1, 0, 2)
    return result.reshape(row_count, group * head_size)


def slots_of(routes, experts, capacity):
    tokens, top_count = routes.shape
    expert_ids = lax.broadcasted_iota(jnp.int32, (tokens, experts), 1)
    named = [(routes[:, k : k + 1] == expert_ids).astype(jnp.float32) for k in range(top_count)]
    earlier = (
        lax.broadcasted_iota(jnp.int32, (tokens, tokens), 1)
        < lax.broadcasted_iota(jnp.int32, (tokens, tokens), 0)
    ).astype(jnp.bfloat16)
    before = jnp.dot(
        earlier, sum(named).astype(jnp.bfloat16), preferred_element_type=jnp.float32
    )
    slot_ids = lax.broadcasted_iota(jnp.int32, (tokens, experts * capacity), 1)
    result = []
    for k in range(top_count):
        rank = jnp.sum(before * named[k], axis=1, keepdims=True).astype(jnp.int32)
        slot = routes[:, k : k + 1] * capacity + rank
        result.append((slot == slot_ids).astype(jnp.float32))
    return result


def dispatch_kernel(tokens_ref, gain_ref, routes_ref, send_ref, normed_ref, *, experts, capacity):
    values32 = tokens_ref[...].astype(jnp.float32)
    normed = (
        values32
        * lax.rsqrt(jnp.mean(values32 * values32, axis=-1, keepdims=True) + epsilon)
        * gain_ref[...]
    ).astype(jnp.bfloat16)
    normed_ref[...] = normed
    chosen = sum(slots_of(routes_ref[...], experts, capacity)).T.astype(jnp.bfloat16)
    send_ref[...] = jnp.dot(chosen, normed, preferred_element_type=jnp.float32).astype(
        jnp.bfloat16
    )


def combine_kernel(routes_ref, weights_ref, *refs, experts, capacity):
    returned_refs, shared_refs, out_ref = refs[:PARTS], refs[PARTS:-1], refs[-1]
    weights = weights_ref[...]
    gates = weights / jnp.sum(weights, axis=-1, keepdims=True) * routed_scale
    chosen = [c.astype(jnp.bfloat16) for c in slots_of(routes_ref[...], experts, capacity)]
    at = 0
    for ref in returned_refs:
        part = pl.ds(at, ref.shape[1])
        total = shared_refs[0][:, part].astype(jnp.float32)
        for shared_ref in shared_refs[1:]:
            total = total + shared_ref[:, part].astype(jnp.float32)
        for k, matrix in enumerate(chosen):
            picked = jnp.dot(matrix, ref[...], preferred_element_type=jnp.float32)
            total = total + gates[:, k : k + 1] * picked
        out_ref[:, part] = total.astype(jnp.bfloat16)
        at += ref.shape[1]


def hidden_of(gate_proj, up_proj):
    return (gate_proj / (1.0 + jnp.exp(-gate_proj)) * up_proj).astype(jnp.bfloat16)


def split_dot(rows, refs):
    total, at = None, 0
    for ref in refs:
        part = jnp.dot(
            rows[:, at : at + ref.shape[0]], ref[...], preferred_element_type=jnp.float32
        )
        total = part if total is None else total + part
        at += ref.shape[0]
    return total


def hidden_kernel(rows_ref, *refs, blocks):
    rows = rows_ref[...]
    for k in range(blocks):
        refs[2 * blocks + k][...] = hidden_of(
            jnp.dot(rows, refs[2 * k][...], preferred_element_type=jnp.float32),
            jnp.dot(rows, refs[2 * k + 1][...], preferred_element_type=jnp.float32),
        )


def hidden_blocks(rows, matrices):
    width = matrices[0][0].shape[1]
    return pl.pallas_call(
        functools.partial(hidden_kernel, blocks=len(matrices)),
        out_shape=[jax.ShapeDtypeStruct((rows.shape[0], width), jnp.bfloat16)] * len(matrices),
        cost_estimate=pl.CostEstimate(
            flops=4 * rows.size * width * len(matrices),
            bytes_accessed=4 * rows.size,
            transcendentals=0,
        ),
        name="hidden",
    )(rows, *sum(matrices, ()))


def down_kernel(*refs, blocks):
    hidden_refs, refs = refs[:blocks], refs[blocks:]
    total, at = None, 0
    for ref in hidden_refs:
        width, weights = 0, []
        while width < ref.shape[1]:
            weights.append(refs[at])
            width += refs[at].shape[0]
            at += 1
        part = split_dot(ref[...], weights).astype(jnp.bfloat16).astype(jnp.float32)
        total = part if total is None else total + part
    refs[-1][...] = total.astype(jnp.bfloat16)


def down_blocks(hidden, w_down):
    rows, width = hidden[0].shape[0], w_down[0].shape[1]
    tile = 512
    return pl.pallas_call(
        functools.partial(down_kernel, blocks=len(hidden)),
        grid=(width // tile,),
        in_specs=[pl.BlockSpec(h.shape, lambda i: (0, 0)) for h in hidden]
        + [pl.BlockSpec((w.shape[0], tile), lambda i: (0, i)) for w in w_down],
        out_specs=pl.BlockSpec((rows, tile), lambda i: (0, i)),
        out_shape=jax.ShapeDtypeStruct((rows, width), jnp.bfloat16),
        cost_estimate=pl.CostEstimate(
            flops=2 * rows * width * hidden[0].shape[1] * len(hidden),
            bytes_accessed=4 * rows * width,
            transcendentals=0,
        ),
        name="down",
    )(*hidden, *w_down)


def shared_kernel(*refs, blocks):
    rows = jnp.concatenate([ref[...] for ref in refs[:blocks]], axis=0)
    w_gate, w_up, w_down = refs[blocks : blocks + 3]
    hidden = hidden_of(
        jnp.dot(rows, w_gate[...], preferred_element_type=jnp.float32),
        jnp.dot(rows, w_up[...], preferred_element_type=jnp.float32),
    )
    part = jnp.dot(hidden, w_down[...], preferred_element_type=jnp.float32).astype(jnp.bfloat16)
    count = refs[0].shape[0]
    for k, out_ref in enumerate(refs[blocks + 3 :]):
        out_ref[...] = part[k * count : (k + 1) * count]


def shared_blocks(rows, w_gate, w_up, w_down):
    return pl.pallas_call(
        functools.partial(shared_kernel, blocks=len(rows)),
        out_shape=tuple(jax.ShapeDtypeStruct(r.shape, jnp.bfloat16) for r in rows),
        cost_estimate=pl.CostEstimate(
            flops=6 * len(rows) * rows[0].shape[0] * w_gate.size,
            bytes_accessed=6 * w_gate.size,
            transcendentals=0,
        ),
        name="shared",
    )(*rows, w_gate, w_up, w_down)


def from_both(own):
    return shifted(own, "tp", 1), shifted(own, "tp", -1)


def experts_half(
    moe_tokens,
    norm_gain,
    routes,
    route_weights,
    expert_gate,
    expert_up,
    expert_down,
    shared_gate,
    shared_up,
    shared_down,
):
    tok_rows, model_width = moe_tokens.shape
    top_count = routes.shape[1]
    experts = expert_gate.shape[0] * lax.axis_size(EP)
    capacity = 2 * tok_rows * top_count // experts
    slots = experts * capacity
    lane = lax.axis_index("tp")
    own_routes = lax.dynamic_slice_in_dim(routes, lane * tok_rows, tok_rows, 0)
    own_weights = lax.dynamic_slice_in_dim(route_weights, lane * tok_rows, tok_rows, 0)

    gate, up, down = expert_gate[0], expert_up[0], expert_down[0]
    gate_back, gate_ahead = from_both(gate)
    up_back, up_ahead = from_both(up)
    gate_opposite = shifted(gate_back, "tp", 1)
    up_opposite = shifted(up_ahead, "tp", -1)
    half = down.shape[0] // 2
    downs = []
    for part in jnp.split(down, PARTS, axis=1):
        back, ahead = from_both(part)
        upper = shifted(back[:half], "tp", 1)
        lower = shifted(ahead[half:], "tp", -1)
        downs.append((part, back, ahead, upper, lower))

    send, normed = pl.pallas_call(
        functools.partial(dispatch_kernel, experts=experts, capacity=capacity),
        out_shape=(
            jax.ShapeDtypeStruct((slots, model_width), jnp.bfloat16),
            jax.ShapeDtypeStruct((tok_rows, model_width), jnp.bfloat16),
        ),
        name="dispatch",
    )(moe_tokens, norm_gain[None], own_routes)

    arrived = lax.all_to_all(
        send.reshape(experts, capacity, model_width), EP, 0, 0, tiled=True
    )
    arrived = arrived.reshape(slots, model_width)

    turns = (1, -1, 2)
    group_rows = [normed] + [shifted(normed, "tp", by) for by in turns]
    own_part, *parts = shared_blocks(group_rows, shared_gate, shared_up, shared_down)
    shared_parts = [own_part] + [shifted(part, "tp", -by) for by, part in zip(turns, parts)]

    near = ((gate, up), (gate_back, up_back), (gate_ahead, up_ahead))
    hidden = hidden_blocks(arrived, near)
    hidden = hidden + hidden_blocks(arrived, ((gate_opposite, up_opposite),))
    returned = []
    for w_down in downs:
        outgoing = down_blocks(hidden, w_down)
        received = lax.all_to_all(
            outgoing.reshape(experts, capacity, -1), EP, 0, 0, tiled=True
        )
        returned.append(received.reshape(slots, -1))
    return pl.pallas_call(
        functools.partial(combine_kernel, experts=experts, capacity=capacity),
        out_shape=jax.ShapeDtypeStruct((tok_rows, model_width), jnp.bfloat16),
        name="combine",
    )(own_routes, own_weights, *returned, *shared_parts)


def body(
    query_rows,
    key_rows,
    value_rows,
    query_gain,
    key_gain,
    moe_tokens,
    norm_gain,
    routes,
    route_weights,
    expert_gate,
    expert_up,
    expert_down,
    shared_gate,
    shared_up,
    shared_down,
):
    attn_out = attend(query_rows, key_rows, value_rows, query_gain, key_gain)
    moe_out = experts_half(
        moe_tokens,
        norm_gain,
        routes,
        route_weights,
        expert_gate,
        expert_up,
        expert_down,
        shared_gate,
        shared_up,
        shared_down,
    )
    return (attn_out, moe_out)


def solution(mesh):
    finer = Mesh(mesh.devices.reshape(8, 4, 2, mesh.shape["tp"]), ("ep_0", "ep_1", "ep_2", "tp"))
    return jax.shard_map(
        body,
        mesh=finer,
        in_specs=(
            P(EP, "tp"),
            P(EP, "tp"),
            P(EP, "tp"),
            P(),
            P(),
            P(EP_TP, None),
            P(),
            P(EP, None),
            P(EP, None),
            P(EP, None, "tp"),
            P(EP, None, "tp"),
            P(EP, "tp", None),
            P(None, "tp"),
            P(None, "tp"),
            P("tp", None),
        ),
        out_specs=(P(EP, "tp"), P(EP_TP, None)),
        check_vma=False,
    )
```
